32 devices in a mesh: ep: 8 (over z, x), tp: 4 (over y, core).
Axes of the slice: x: 2, y: 2, z: 4, core: 2. Of those that a mesh axis runs over, the one named last changes fastest.
Arguments:
- queries: bfloat16 [2048, 2048], P('ep', 'tp'), may hold values from -9 to 9
- key_rows: bfloat16 [2048, 2048], P('ep', 'tp'), may hold values from -9 to 9
- values: bfloat16 [2048, 2048], P('ep', 'tp'), may hold values from -6 to 6
- second_scale: float32 [16], P('tp'), may hold values from 0.3 to 0.8
- head_gain: float32 [128], replicated, may hold values from 0.1 to 1.9
- out_weight: bfloat16 [2048, 2048], P(None, 'tp'), may hold values from -0.125 to 0.125
- routed_in: bfloat16 [2048, 2048], P('ep'), may hold values from -6 to 6
- routed_gain: float32 [2048], replicated, may hold values from 0.1 to 1.9
- expert_ids: int32 [2048, 2], P('ep'), may hold values from 0 to 7, all different within a row; in each aligned block of 256 rows (0 to 255, 256 to 511, ...) at most 128 rows name the same one
- group_logits: float32 [2048, 2], P('ep'), may hold values from -6 to 6
- inner_logits: float32 [2048, 2], P('ep'), may hold values from -6 to 6
- gate_weight: bfloat16 [8, 2048, 4096], P('ep', None, 'tp'), may hold values from -0.125 to 0.125
- up_weight: bfloat16 [8, 2048, 4096], P('ep', None, 'tp'), may hold values from -0.125 to 0.125
- down_weight: bfloat16 [8, 4096, 2048], P('ep', 'tp'), may hold values from -0.09375 to 0.09375
Outputs:
- mixer_out: bfloat16 [2048, 2048], P('ep', 'tp')
- routed_out: bfloat16 [2048, 2048], P('ep', 'tp')
The draws below stay inside these ranges and needn't reach their ends.
Inputs may be any that keep to these rules, and one draw needn't show every extreme that they name: `expert_ids`: the two ids of a row differ. In the rows of one device (aligned blocks of 256 rows) no expert is named by more than 128 rows, a bound that some block reaches.
All inputs are finite; a program needn't handle non-finite values.
Results may differ from the reference program's by a relative error of at most 0.018.
Values may be sent and summed in bfloat16 or wider, within the bound.
A program may use at most 128 MiB of HBM per device.

```python
import math
import jax
import jax.numpy as jnp
import numpy as np
from jax import lax

D = 2048
HEADS = 16
QK = 64
VD = 128
FF = 4096
TOPK = 2
GROUP_SIZE = 4
TM = 256
LA = 2048
TOKM = 2048
EXPERTS = 8
GROUPS = 2
CAP = 128
N_EP = 8
N_TP = 4


def base_field(key):
    spread = 1.32
    return jnp.clip(jax.random.normal(key, (LA, HEADS * 2 * QK), jnp.float32) * spread, -8.0, 8.0)


def draw_queries(key, part):
    field = base_field(jax.random.fold_in(key, 1))
    return field.astype(jnp.bfloat16)


def draw_key_rows(key, part):
    field = base_field(jax.random.fold_in(key, 2))
    return field.astype(jnp.bfloat16)


def level_of(key, dims, cuts, low, high):
    level, own = 1.0, jax.random.fold_in(key, 6)
    for axis_at, blocks in cuts:
        heights = jnp.exp(jax.random.uniform(jax.random.fold_in(own, axis_at), (blocks,), jnp.float32, low / len(cuts), high / len(cuts)))
        level = level * jnp.repeat(heights, dims[axis_at] // blocks).reshape([-1 if axis == axis_at else 1 for axis in range(len(dims))])
    return level


def shared_out(rng, own, number, rows, amount, top, most, slope):
    sequence = jax.random.permutation(rng, amount)
    heavy_load, ordinary = load_shares(amount, rows * top, most, slope, True), load_shares(amount, rows * top, most, slope, False)
    places = jnp.arange(amount)

    def named(tallies, rotation):
        used = int((tallies > 0).sum())
        fixed = max(1, used // 4)
        moved = fixed + (places - fixed + rotation * (used - fixed)) % max(1, amount - fixed)
        return jnp.zeros((amount,), jnp.int32).at[sequence[jnp.where(places < fixed, places, moved)]].set(jnp.asarray(tallies, jnp.int32))

    tallies = jnp.where(number % 4 == 0, named(heavy_load, number // 4), named(ordinary, number - number // 4 - 1))
    mixed = jax.random.permutation(jax.random.fold_in(own, 3), amount)
    donor, taker = mixed[0:amount // 2 * 2:2], mixed[1:amount // 2 * 2:2]
    room = jnp.minimum(tallies[donor] - 1, most - tallies[taker]) // 2
    room = jnp.where((donor == sequence[0]) | (taker == sequence[0]) | (tallies[taker] == 0), 0, jnp.maximum(room, 0))
    moved = jax.random.randint(jax.random.fold_in(own, 4), (amount // 2,), 0, 1 << 20) % (room + 1)
    tallies = tallies.at[donor].add(-moved).at[taker].add(moved)
    items = jnp.searchsorted(jnp.cumsum(tallies), jnp.arange(rows * top), side="right").astype(jnp.int32)
    listing = items.reshape(top, rows).T
    listing = listing[jax.random.permutation(jax.random.fold_in(own, 1), rows)]
    rotation = jax.random.randint(jax.random.fold_in(own, 2), (rows, 1), 0, top)
    return jnp.take_along_axis(listing, (jnp.arange(top)[None, :] + rotation) % top, axis=1)


def load_shares(number_of, total, reach, skew, full):
    loads = [(1 << 20) // math.isqrt(standing ** skew) + 1 for standing in range(1, number_of + 1)]
    largest = reach if full else min(reach, max(-(-total // number_of), total * loads[0] // sum(loads)))
    least = 1 if total - largest >= number_of - 1 else 0
    given, surplus = [largest] + [least] * (number_of - 1), total - largest - least * (number_of - 1)
    while surplus > 0:
        free = [i for i in range(1, number_of) if given[i] < largest] or [i for i in range(1, number_of) if given[i] < reach]
        whole, budget = sum([loads[i] for i in free]), surplus
        for i in free:
            addition = min(reach - given[i], max(1, budget * loads[i] // whole), surplus)
            given[i] = given[i] + addition
            surplus = surplus - addition
    return np.array(given)


def gaussian(own_key, extent, width, bound, pieces=(), held_as=jnp.bfloat16):
    entries = jax.random.normal(own_key, extent, jnp.float32) * width
    if len(pieces) > 0:
        entries = level_of(own_key, extent, pieces, -0.22, 0.18) * entries
    return jnp.clip(entries, min=-bound, max=bound).astype(held_as)


def setup_inputs(seed: int = 0) -> dict:
    seeds = jax.random.split(jax.random.key(seed), 15)
    queries = draw_queries(jax.random.fold_in(seeds[14], 71), 0)
    key_rows = draw_key_rows(jax.random.fold_in(seeds[14], 71), 0)
    values = gaussian(seeds[2], (LA, HEADS * VD), 1.0, 6.0, ((0, 8), (1, 4)))
    second_scale = jnp.clip(0.3 + 0.5 * jax.random.uniform(seeds[3], (HEADS,), jnp.float32) ** level_of(seeds[3], (HEADS,), ((0, 4),), -0.2, 0.2), 0.3, 0.8)
    head_gain = jnp.clip(1.0 + 0.18 * jax.random.normal(seeds[4], (VD,), jnp.float32), 0.1, 1.9)
    out_weight = gaussian(seeds[5], (HEADS * VD, D), (HEADS * VD) ** -0.5, 0.125, ((1, 4),))
    routed_in = gaussian(seeds[6], (TOKM, D), 1.0, 6.0, ((0, 8),))
    routed_gain = jnp.clip(1.0 + 0.18 * jax.random.normal(seeds[7], (D,), jnp.float32), 0.1, 1.9)
    expert_ids_keys = jax.random.split(jax.random.fold_in(seeds[8], 1), TOKM // TM)
    expert_ids_turns = jax.random.permutation(jax.random.fold_in(seeds[8], 3), TOKM // TM)
    expert_ids = jax.vmap(lambda own, number: shared_out(jax.random.fold_in(seeds[8], 2), own, number, TM, EXPERTS, TOPK, CAP, 2))(expert_ids_keys, expert_ids_turns).reshape((TOKM, TOPK))
    group_logits = gaussian(seeds[9], (TOKM, GROUPS), 1.5, 6.0, ((0, 8),), jnp.float32)
    inner_logits = gaussian(seeds[10], (TOKM, TOPK), 1.0, 6.0, ((0, 8),), jnp.float32)
    gate_weight = gaussian(seeds[11], (EXPERTS, D, FF), D ** -0.5, 0.125, ((0, 8), (2, 4)))
    up_weight = gaussian(seeds[12], (EXPERTS, D, FF), D ** -0.5, 0.125, ((0, 8), (2, 4)))
    down_weight = gaussian(seeds[13], (EXPERTS, FF, D), FF ** -0.5, 0.09375, ((0, 8), (1, 4)))
    return {"queries": queries, "key_rows": key_rows, "values": values, "second_scale": second_scale, "head_gain": head_gain, "out_weight": out_weight, "routed_in": routed_in, "routed_gain": routed_gain, "expert_ids": expert_ids, "group_logits": group_logits, "inner_logits": inner_logits, "gate_weight": gate_weight, "up_weight": up_weight, "down_weight": down_weight}


EPSILON = 1e-05

def head_block(query_block, key_block, value_block, scale_head, first_pos):
    scores = jnp.einsum('qmd,kmd->mqk', query_block, key_block) * QK ** (-0.5)
    query_pos = first_pos + jnp.arange(query_block.shape[0], dtype=jnp.int32)
    key_pos = jnp.arange(key_block.shape[0], dtype=jnp.int32)
    visible = query_pos[:, None] >= key_pos[None, :]
    scores = jnp.where(visible, scores, -jnp.inf)
    row_max = lax.optimization_barrier(jnp.max(scores, axis=-1, keepdims=True))
    exp_terms = jnp.exp(scores - row_max)
    denominator = lax.optimization_barrier(jnp.sum(exp_terms, axis=-1))
    rounded = lax.optimization_barrier(exp_terms.astype(jnp.bfloat16)).astype(jnp.float32)
    weighted = jnp.einsum('mqk,ke->mqe', rounded, value_block)
    mapped = weighted / denominator[..., None]
    return mapped[0] - scale_head * mapped[1]

def reference(queries, key_rows, values, second_scale, head_gain, out_weight, routed_in, routed_gain, expert_ids, group_logits, inner_logits, gate_weight, up_weight, down_weight):
    query_all = jnp.transpose(queries.astype(jnp.float32).reshape(LA, HEADS, 2, QK), (1, 0, 2, 3))
    key_all = jnp.transpose(key_rows.astype(jnp.float32).reshape(LA, HEADS, 2, QK), (1, 0, 2, 3))
    value_all = jnp.transpose(values.astype(jnp.float32).reshape(LA, HEADS, VD), (1, 0, 2))
    block_rows = min(512, LA)
    outputs = []
    for first_pos in range(0, LA, block_rows):
        limit = first_pos + block_rows

        def per_head(operands, first_pos=first_pos):
            query_head, key_head, value_head, scale_head = operands
            return head_block(query_head, key_head, value_head, scale_head, first_pos)
        outputs.append(lax.map(per_head, (query_all[:, first_pos:limit], key_all[:, :limit], value_all[:, :limit], second_scale)))
    difference = jnp.concatenate(outputs, axis=1)
    inv_norm = lax.rsqrt(lax.optimization_barrier(jnp.mean(difference * difference, axis=-1, keepdims=True)) + EPSILON)
    head_out = (difference * inv_norm * head_gain).astype(jnp.bfloat16)
    head_out = jnp.transpose(head_out, (1, 0, 2)).reshape(LA, HEADS * VD)
    mixer_out = jnp.dot(head_out, out_weight, preferred_element_type=jnp.float32).astype(jnp.bfloat16)
    source = routed_in.astype(jnp.float32)
    normed = (source * lax.rsqrt(lax.optimization_barrier(jnp.mean(source * source, axis=-1, keepdims=True)) + EPSILON) * routed_gain).astype(jnp.bfloat16)
    block_ids = expert_ids.reshape(N_EP, TM * TOPK)
    picked = (block_ids[..., None] == jnp.arange(EXPERTS, dtype=jnp.int32)).astype(jnp.int32)
    slot_index = lax.optimization_barrier(jnp.sum(jnp.cumsum(picked, axis=1) * picked, axis=-1)) - 1
    place_index = (jnp.arange(N_EP, dtype=jnp.int32)[:, None] * CAP + slot_index).reshape(-1).astype(jnp.int32)
    flat_ids = expert_ids.reshape(-1).astype(jnp.int32)
    owner_row = (jnp.arange(TOKM * TOPK, dtype=jnp.int32) // TOPK).astype(jnp.int32)
    slot_rows = jnp.zeros((EXPERTS, N_EP * CAP), jnp.int32).at[flat_ids, place_index].set(owner_row)

    def one_expert(operands):
        rows_of, gate_part, up_part, down_part = operands
        gathered = normed[rows_of]
        gate_act = jnp.dot(gathered, gate_part, preferred_element_type=jnp.float32)
        up_act = jnp.dot(gathered, up_part, preferred_element_type=jnp.float32)
        hidden = (jax.nn.silu(gate_act) * up_act).astype(jnp.bfloat16)
        split_hidden = hidden.reshape(N_EP * CAP, N_TP, FF // N_TP).astype(jnp.float32)
        split_down = down_part.reshape(N_TP, FF // N_TP, D).astype(jnp.float32)
        partial_value = jnp.einsum('rtf,tfd->trd', split_hidden, split_down)
        rounded = lax.optimization_barrier(partial_value.astype(jnp.bfloat16)).astype(jnp.float32)
        return lax.optimization_barrier(jnp.sum(rounded, axis=0)).astype(jnp.bfloat16)
    expert_out = lax.map(one_expert, (slot_rows, gate_weight, up_weight, down_weight))
    pair_out = expert_out[flat_ids, place_index].reshape(TOKM, TOPK, D)
    group_prob = jax.nn.softmax(group_logits, axis=-1)
    member = (expert_ids[..., None] // GROUP_SIZE == jnp.arange(GROUPS, dtype=jnp.int32)).astype(jnp.float32)
    group_pick = lax.optimization_barrier(jnp.sum(group_prob[:, None, :] * member, axis=-1))
    route_weight = group_pick * jax.nn.softmax(inner_logits, axis=-1)
    routed_out = lax.optimization_barrier(jnp.sum(route_weight[..., None] * pair_out.astype(jnp.float32), axis=1)).astype(jnp.bfloat16)
    return (mixer_out, routed_out)
```

```python
import functools
import math

import jax
import jax.numpy as jnp
from jax import lax
from jax.experimental import pallas as pl
from jax.experimental.pallas import tpu as pltpu
from jax.sharding import PartitionSpec as P

GROUP_SIZE = 4


EPSILON = 1e-05
LOWEST = -1e30


def token_mixer(queries, key_rows, values, second_scale, head_gain, out_weight):
    row_count = queries.shape[0]
    local_heads = second_scale.shape[0]
    qk_size = queries.shape[1] // (2 * local_heads)
    value_size = values.shape[1] // local_heads
    first_pos = lax.axis_index("ep") * row_count
    query_pos = first_pos + jnp.arange(row_count, dtype=jnp.int32)
    last_pos = first_pos + row_count - 1
    query_four = queries.reshape(row_count, local_heads, 2, qk_size)
    score_scale = qk_size ** (-0.5)
    initial = (
        jnp.full((row_count, local_heads, 2), LOWEST, jnp.float32),
        jnp.zeros((row_count, local_heads, 2), jnp.float32),
        jnp.zeros((row_count, local_heads, 2, value_size), jnp.float32),
    )
    state_now = initial
    key_piece = lax.all_gather(key_rows, "ep", axis=0, tiled=True)
    value_piece = lax.all_gather(values, "ep", axis=0, tiled=True)
    piece_count = key_piece.shape[0]
    block_width = math.gcd(piece_count, 512)
    blocks = piece_count // block_width
    key_blocks = key_piece.reshape(blocks, block_width, local_heads, 2, qk_size)
    value_blocks = value_piece.reshape(blocks, block_width, local_heads, value_size)

    def update(state_inner, block_index):
        key_start = block_index * block_width

        def attend(inner_state):
            running_max, denominator, weighted = inner_state
            scores = (
                jnp.einsum(
                    "qhmd,khmd->qhmk",
                    query_four,
                    key_blocks[block_index],
                    preferred_element_type=jnp.float32,
                )
                * score_scale
            )
            key_pos = key_start + jnp.arange(block_width, dtype=jnp.int32)
            visible = (query_pos[:, None] >= key_pos[None, :])[:, None, None, :]
            scores = jnp.where(visible, scores, LOWEST)
            new_max = jnp.maximum(running_max, jnp.max(scores, axis=-1))
            exp_terms = jnp.where(visible, jnp.exp(scores - new_max[..., None]), 0.0)
            factor = jnp.exp(running_max - new_max)
            denominator = denominator * factor + jnp.sum(exp_terms, axis=-1)
            weighted = weighted * factor[..., None] + jnp.einsum(
                "qhmk,khe->qhme",
                exp_terms.astype(jnp.bfloat16),
                value_blocks[block_index],
                preferred_element_type=jnp.float32,
            )
            return (new_max, denominator, weighted)

        return (
            lax.cond(key_start <= last_pos, attend, lambda inner_state: inner_state, state_inner),
            None,
        )

    state_now, _ = lax.scan(update, state_now, jnp.arange(blocks, dtype=jnp.int32))
    running_max, denominator, weighted = state_now
    mapped = weighted / denominator[..., None]
    difference = mapped[:, :, 0] - second_scale[None, :, None] * mapped[:, :, 1]
    inv_norm = lax.rsqrt(jnp.mean(difference * difference, axis=-1, keepdims=True) + EPSILON)
    head_out = (
        (difference * inv_norm * head_gain)
        .astype(jnp.bfloat16)
        .reshape(row_count, local_heads * value_size)
    )
    mixed = jnp.dot(
        lax.all_gather(head_out, "tp", axis=1, tiled=True),
        out_weight,
        preferred_element_type=jnp.float32,
    )
    return mixed.astype(jnp.bfloat16)


MESH = pl.DeviceIdType.MESH


def moe_kernel(
    sizes,
    out_ref,
    gate_hbm,
    up_hbm,
    down_hbm,
    ret_ref,
    gate_ref,
    up_ref,
    down_ref,
    arr,
    hidden,
    own_sum,
    sib_send,
    sib_recv,
    y_send,
    y_recv,
    answer,
    w_sem,
    a_send,
    a_recv,
    b_send,
    b_recv,
    s_send,
    s_recv,
    y_ssem,
    y_rsem,
    r_send,
    r_recv,
):
    n_ep, n_tp, cap, cols = sizes
    pairs, n_y = n_ep // 2, n_tp // 2
    me, tp = lax.axis_index("ep"), lax.axis_index("tp")
    my_pair, half = me // 2, lax.rem(me, 2)
    my_y, core = tp // 2, lax.rem(tp, 2)
    sib = my_y * 2 + 1 - core

    def wcopy(i, src, dst):
        return pltpu.make_async_copy(src.at[0], dst, w_sem.at[i])

    weights = [wcopy(0, gate_hbm, gate_ref), wcopy(1, up_hbm, up_ref), wcopy(2, down_hbm, down_ref)]
    for copy in weights:
        copy.start()

    barrier = pltpu.get_barrier_semaphore()
    for d in range(1, n_ep):
        pl.semaphore_signal(
            barrier, inc=1, device_id={"ep": lax.rem(me + d, n_ep), "tp": tp}, device_id_type=MESH
        )
    for d in range(1, n_tp):
        pl.semaphore_signal(
            barrier, inc=1, device_id={"ep": me, "tp": lax.rem(tp + d, n_tp)}, device_id_type=MESH
        )
    pl.semaphore_wait(barrier, n_ep - 1 + n_tp - 1)

    def remote(src, dst, ssem, rsem, ep, tpi):
        return pltpu.make_async_remote_copy(
            src_ref=src,
            dst_ref=dst,
            send_sem=ssem,
            recv_sem=rsem,
            device_id={"ep": ep, "tp": tpi},
            device_id_type=MESH,
        )

    def lanes(t):
        return pl.ds(pl.multiple_of(t * cols, cols), cols)

    def rows(h):
        return pl.ds(pl.multiple_of(h * cap, cap), cap)

    def block(ref, n, t):
        return ref.at[n // 2, rows(lax.rem(n, 2)), lanes(t)]

    def a_copy(dest, src_n):
        return remote(out_ref.at[dest], block(arr, src_n, tp), a_send.at[dest], a_recv.at[src_n], dest, tp)

    def dispatch(d, carry):
        pair = lax.rem(my_pair - d + pairs, pairs)
        for h in range(2):
            dest = pair * 2 + h

            @pl.when(dest != me)
            def _():
                a_copy(dest, me).start()

            @pl.when(dest == me)
            def _():
                arr[my_pair, rows(half), lanes(tp)] = out_ref[me]

        return carry

    lax.fori_loop(0, pairs, dispatch, 0)

    def b_copy(p, t, to, k):
        return remote(
            arr.at[p, :, lanes(t)], arr.at[p, :, lanes(t)], b_send.at[p, k], b_recv.at[p, t], me, to
        )

    def gather_pair(p):
        for h in range(2):
            n = p * 2 + h

            @pl.when(n != me)
            def _():
                a_copy(n, n).wait_recv()

        for dy in range(1, n_y):
            to = lax.rem(my_y + dy, n_y) * 2 + core
            b_copy(p, tp, to, dy - 1).start()
        b_copy(p, tp, sib, n_y - 1).start()

    def forward_pair(p):
        for dy in range(1, n_y):
            t = lax.rem(my_y + n_y - dy, n_y) * 2 + core
            b_copy(p, t, t, 0).wait_recv()
            b_copy(p, t, sib, n_y - 1 + dy).start()
        b_copy(p, sib, sib, 0).wait_recv()
        for dy in range(1, n_y):
            t = lax.rem(my_y + n_y - dy, n_y) * 2 + 1 - core
            b_copy(p, t, sib, 0).wait_recv()

    ff = gate_ref.shape[1]
    tile = min(256, ff)

    def s_copy(p):
        return remote(sib_send.at[p], sib_recv.at[p], s_send.at[p], s_recv.at[p], me, sib)

    def y_copy(p, dy):
        to = lax.rem(my_y + dy, n_y) * 2 + core
        return remote(
            y_send.at[p, dy - 1], y_recv.at[p, dy - 1], y_ssem.at[p, dy - 1], y_rsem.at[p, dy - 1], me, to
        )

    def compute(p):
        def up_tile(f, carry):
            at = pl.ds(pl.multiple_of(f * tile, tile), tile)
            x = arr[p]
            gate = jnp.dot(x, gate_ref[:, at], preferred_element_type=jnp.float32)
            up = jnp.dot(x, up_ref[:, at], preferred_element_type=jnp.float32)
            hidden[:, at] = (gate / (1.0 + jnp.exp(-gate)) * up).astype(jnp.bfloat16)
            return carry

        lax.fori_loop(0, ff // tile, up_tile, 0)

        def sib_tile(y, carry):
            part = jnp.dot(
                hidden[...], down_ref[:, lanes(y * 2 + 1 - core)], preferred_element_type=jnp.float32
            )
            sib_send[p, y] = part.astype(jnp.bfloat16)
            return carry

        lax.fori_loop(0, n_y, sib_tile, 0)
        s_copy(p).start()

        def own_tile(y, carry):
            own_sum[p, y] = jnp.dot(
                hidden[...], down_ref[:, lanes(y * 2 + core)], preferred_element_type=jnp.float32
            )
            return carry

        lax.fori_loop(0, n_y, own_tile, 0)

    def chip_sum(p):
        s_copy(p).wait_recv()
        for dy in range(1, n_y):
            y = lax.rem(my_y + dy, n_y)
            y_send[p, dy - 1] = (own_sum[p, y] + sib_recv[p, y].astype(jnp.float32)).astype(jnp.bfloat16)
            y_copy(p, dy).start()

    def r_copy(dest, src_n):
        return remote(
            answer.at[dest // 2, rows(lax.rem(dest, 2))], ret_ref.at[src_n], r_send.at[dest], r_recv.at[src_n], dest, tp
        )

    def give_back(p):
        total = own_sum[p, my_y] + sib_recv[p, my_y].astype(jnp.float32)
        for dy in range(1, n_y):
            y_copy(p, dy).wait_recv()
            total = total + y_recv[p, dy - 1].astype(jnp.float32)
        answer[p] = total.astype(jnp.bfloat16)
        for h in range(2):
            dest = p * 2 + h

            @pl.when(dest != me)
            def _():
                r_copy(dest, me).start()

            @pl.when(dest == me)
            def _():
                ret_ref[me] = answer[my_pair, rows(half)]

    def pair_of(d):
        return lax.rem(my_pair + d + pairs, pairs)

    def step(i, carry):
        @pl.when(i < pairs)
        def _():
            gather_pair(pair_of(i))

        @pl.when(jnp.logical_and(i >= LAG, i < pairs + LAG))
        def _():
            p = pair_of(i - LAG)
            forward_pair(p)

            @pl.when(i == LAG)
            def _():
                for copy in weights:
                    copy.wait()

            compute(p)

        @pl.when(jnp.logical_and(i >= LAG + 1, i < pairs + LAG + 1))
        def _():
            chip_sum(pair_of(i - LAG - 1))

        @pl.when(i >= LAG + 2)
        def _():
            give_back(pair_of(i - LAG - 2))

        return carry

    lax.fori_loop(0, pairs + LAG + 2, step, 0)

    def drain(d, carry):
        p = pair_of(d)
        for k in range(n_tp - 1):
            b_copy(p, tp, sib, k).wait_send()
        s_copy(p).wait_send()
        for dy in range(1, n_y):
            y_copy(p, dy).wait_send()
        for h in range(2):
            n = p * 2 + h

            @pl.when(n != me)
            def _():
                a_copy(n, n).wait_send()
                r_copy(n, n).wait()

        return carry

    lax.fori_loop(0, pairs, drain, 0)


LAG = 1


def expert_exchange(outgoing, gate_weight, up_weight, down_weight):
    n_ep, cap, cols = outgoing.shape
    n_tp = lax.axis_size("tp")
    width, ff = gate_weight.shape[1:]
    pairs, n_y = n_ep // 2, n_tp // 2
    bf, dma = jnp.bfloat16, pltpu.SemaphoreType.DMA
    return pl.pallas_call(
        functools.partial(moe_kernel, (n_ep, n_tp, cap, cols)),
        out_shape=jax.ShapeDtypeStruct((n_ep, cap, cols), bf),
        in_specs=[pl.BlockSpec(memory_space=pltpu.VMEM)] + [pl.BlockSpec(memory_space=pl.ANY)] * 3,
        out_specs=pl.BlockSpec(memory_space=pltpu.VMEM),
        scratch_shapes=[
            pltpu.VMEM((width, ff), bf),
            pltpu.VMEM((width, ff), bf),
            pltpu.VMEM((ff, width), bf),
            pltpu.VMEM((pairs, 2 * cap, width), bf),
            pltpu.VMEM((2 * cap, ff), bf),
            pltpu.VMEM((pairs, n_y, 2 * cap, cols), jnp.float32),
            pltpu.VMEM((pairs, n_y, 2 * cap, cols), bf),
            pltpu.VMEM((pairs, n_y, 2 * cap, cols), bf),
            pltpu.VMEM((pairs, n_y - 1, 2 * cap, cols), bf),
            pltpu.VMEM((pairs, n_y - 1, 2 * cap, cols), bf),
            pltpu.VMEM((pairs, 2 * cap, cols), bf),
            dma((3,)),
            dma((n_ep,)),
            dma((n_ep,)),
            dma((pairs, n_tp - 1)),
            dma((pairs, n_tp)),
            dma((pairs,)),
            dma((pairs,)),
            dma((pairs, n_y - 1)),
            dma((pairs, n_y - 1)),
            dma((n_ep,)),
            dma((n_ep,)),
        ],
        compiler_params=pltpu.CompilerParams(
            collective_id=0, has_side_effects=True, vmem_limit_bytes=48 * 1024 * 1024
        ),
    )(outgoing, gate_weight, up_weight, down_weight)


def expert_block(
    routed_in,
    routed_gain,
    expert_ids,
    group_logits,
    inner_logits,
    gate_weight,
    up_weight,
    down_weight,
):
    token_count, width = routed_in.shape
    chosen = expert_ids.shape[1]
    ep_size = lax.axis_size("ep")
    capacity = 2 * chosen * token_count // ep_size
    source = routed_in.astype(jnp.float32)
    inv_norm = lax.rsqrt(jnp.mean(source * source, axis=-1, keepdims=True) + EPSILON)
    columns = width // lax.axis_size("tp")
    first = lax.axis_index("tp") * columns
    own_source = lax.dynamic_slice_in_dim(routed_in, first, columns, 1).astype(jnp.float32)
    own_gain = lax.dynamic_slice_in_dim(routed_gain, first, columns, 0)
    normed = (own_source * inv_norm * own_gain).astype(jnp.bfloat16)
    experts = jnp.arange(ep_size, dtype=jnp.int32)
    picks = expert_ids[..., None] == experts
    picked = jnp.any(picks, axis=1)
    positions = jnp.arange(token_count, dtype=jnp.int32)
    before = (positions[:, None] > positions[None, :]).astype(jnp.bfloat16)
    slot = jnp.dot(before, picked.astype(jnp.bfloat16), preferred_element_type=jnp.float32)
    slot = jnp.where(picked, slot.astype(jnp.int32), -1)
    slots = jnp.arange(capacity, dtype=jnp.int32)
    place = slot.T[:, None, :] == slots[None, :, None]
    spread = place.reshape(ep_size * capacity, token_count).astype(jnp.bfloat16)
    outgoing = jnp.dot(spread, normed, preferred_element_type=jnp.float32).astype(jnp.bfloat16)
    returned = expert_exchange(
        outgoing.reshape(ep_size, capacity, columns), gate_weight, up_weight, down_weight
    )
    group_prob = jax.nn.softmax(group_logits, axis=-1)
    member = (
        expert_ids[..., None] // GROUP_SIZE == jnp.arange(group_logits.shape[1], dtype=jnp.int32)
    ).astype(jnp.float32)
    group_pick = jnp.sum(group_prob[:, None, :] * member, axis=-1)
    route_weight = group_pick * jax.nn.softmax(inner_logits, axis=-1)
    expert_weight = jnp.sum(route_weight[..., None] * picks.astype(jnp.float32), axis=1)
    high = expert_weight.astype(jnp.bfloat16)
    low = (expert_weight - high.astype(jnp.float32)).astype(jnp.bfloat16)
    back = slot[:, :, None] == slots[None, None, :]

    def combine(weight):
        mix = jnp.where(back, weight[:, :, None], jnp.bfloat16(0)).reshape(token_count, -1)
        return jnp.dot(mix, returned.reshape(-1, columns), preferred_element_type=jnp.float32)

    return (combine(high) + combine(low)).astype(jnp.bfloat16)


def local(
    queries,
    key_rows,
    values,
    second_scale,
    head_gain,
    out_weight,
    routed_in,
    routed_gain,
    expert_ids,
    group_logits,
    inner_logits,
    gate_weight,
    up_weight,
    down_weight,
):
    mixer_out = token_mixer(queries, key_rows, values, second_scale, head_gain, out_weight)
    routed_out = expert_block(
        routed_in,
        routed_gain,
        expert_ids,
        group_logits,
        inner_logits,
        gate_weight,
        up_weight,
        down_weight,
    )
    return (mixer_out, routed_out)


def solution(mesh):
    return jax.shard_map(
        local,
        mesh=mesh,
        in_specs=(
            P("ep", "tp"),
            P("ep", "tp"),
            P("ep", "tp"),
            P("tp"),
            P(),
            P(None, "tp"),
            P("ep", None),
            P(),
            P("ep", None),
            P("ep", None),
            P("ep", None),
            P("ep", None, "tp"),
            P("ep", None, "tp"),
            P("ep", "tp", None),
        ),
        out_specs=(P("ep", "tp"), P("ep", "tp")),
        check_vma=False,
    )
```

```python
import functools

import jax
import jax.numpy as jnp
from jax import lax
from jax.experimental import pallas as pl
from jax.experimental.pallas import tpu as pltpu
from jax.sharding import PartitionSpec as P

GROUP_SIZE = 4


EPSILON = 1e-05
LOWEST = -1e30


MESH = pl.DeviceIdType.MESH


def fused_kernel(
    sizes,
    out_ref,
    q_ref,
    k_ref,
    v_ref,
    scale_ref,
    gain_ref,
    mix_hbm,
    gate_hbm,
    up_hbm,
    down_hbm,
    ret_ref,
    mixed_ref,
    gate_ref,
    up_ref,
    down_ref,
    arr,
    hidden,
    own_sum,
    sib_send,
    sib_recv,
    y_send,
    y_recv,
    answer,
    w_sem,
    a_send,
    a_recv,
    b_send,
    b_recv,
    s_send,
    s_recv,
    y_ssem,
    y_rsem,
    r_send,
    r_recv,
    mix_ref,
    kbuf,
    vbuf,
    qbuf,
    qtwo,
    hsend,
    heads,
    k_send,
    k_recv,
    q_send,
    q_recv,
    o_send,
    o_recv,
    g_send,
    g_recv,
):
    n_ep, n_tp, cap, cols, n_head = sizes
    pairs, n_y = n_ep // 2, n_tp // 2
    me, tp = lax.axis_index("ep"), lax.axis_index("tp")
    my_pair, half = me // 2, lax.rem(me, 2)
    my_y, core = tp // 2, lax.rem(tp, 2)
    sib = my_y * 2 + 1 - core

    def wcopy(i, src, dst):
        return pltpu.make_async_copy(src, dst, w_sem.at[i])

    weights = [
        wcopy(0, gate_hbm.at[0], gate_ref),
        wcopy(1, up_hbm.at[0], up_ref),
        wcopy(2, down_hbm.at[0], down_ref),
        wcopy(3, mix_hbm, mix_ref),
    ]
    for copy in weights:
        copy.start()

    barrier = pltpu.get_barrier_semaphore()
    for d in range(1, n_ep):
        pl.semaphore_signal(
            barrier, inc=1, device_id={"ep": lax.rem(me + d, n_ep), "tp": tp}, device_id_type=MESH
        )
    for d in range(1, n_tp):
        pl.semaphore_signal(
            barrier, inc=1, device_id={"ep": me, "tp": lax.rem(tp + d, n_tp)}, device_id_type=MESH
        )
    pl.semaphore_wait(barrier, n_ep - 1 + n_tp - 1)

    def remote(src, dst, ssem, rsem, ep, tpi):
        return pltpu.make_async_remote_copy(
            src_ref=src,
            dst_ref=dst,
            send_sem=ssem,
            recv_sem=rsem,
            device_id={"ep": ep, "tp": tpi},
            device_id_type=MESH,
        )

    def lanes(t):
        return pl.ds(pl.multiple_of(t * cols, cols), cols)

    def rows(h):
        return pl.ds(pl.multiple_of(h * cap, cap), cap)

    def block(ref, n, t):
        return ref.at[n // 2, rows(lax.rem(n, 2)), lanes(t)]

    def a_copy(dest, src_n):
        return remote(out_ref.at[dest], block(arr, src_n, tp), a_send.at[dest], a_recv.at[src_n], dest, tp)

    def dispatch(d, carry):
        pair = lax.rem(my_pair - d + pairs, pairs)
        for h in range(2):
            dest = pair * 2 + h

            @pl.when(dest != me)
            def _():
                a_copy(dest, me).start()

            @pl.when(dest == me)
            def _():
                arr[my_pair, rows(half), lanes(tp)] = out_ref[me]

        return carry

    lax.fori_loop(0, pairs, dispatch, 0)

    n_part = n_ep // n_head
    row_of, part = me // n_part, lax.rem(me, n_part)
    my_group = part + lax.rem(row_of, 2) * (n_part - 1 - 2 * part)
    row_count, wide = qbuf.shape[1:]
    value_size = vbuf.shape[2]

    def wide_at(h, size):
        return pl.ds(pl.multiple_of(h * size, size), size)

    def kv_copies(ksrc, vsrc, n, dest, k):
        return (
            remote(ksrc, kbuf.at[n], k_send.at[0, k], k_recv.at[0, n], dest, tp),
            remote(vsrc, vbuf.at[n], k_send.at[1, k], k_recv.at[1, n], dest, tp),
        )

    def kv_first(d):
        head = lax.rem(row_of + d, n_head)
        return kv_copies(
            k_ref.at[:, wide_at(head, wide)],
            v_ref.at[:, wide_at(head, value_size)],
            me,
            head * n_part + part,
            d,
        )

    def kv_second(r, ds):
        n = r * n_part + part
        dest = row_of * n_part + lax.rem(part + ds, n_part)
        return kv_copies(kbuf.at[n], vbuf.at[n], n, dest, n_head + r * (n_part - 1) + ds - 1)

    def kv_own(ds):
        n = me
        dest = row_of * n_part + lax.rem(part + ds, n_part)
        return kv_copies(
            k_ref.at[:, wide_at(row_of, wide)],
            v_ref.at[:, wide_at(row_of, value_size)],
            n,
            dest,
            n_head + row_of * (n_part - 1) + ds - 1,
        )

    def q_copy(d):
        head = lax.rem(row_of + d, n_head)
        return remote(
            q_ref.at[:, wide_at(head, wide)],
            qbuf.at[row_of],
            q_send.at[d],
            q_recv.at[row_of],
            head * n_part + my_group,
            tp,
        )

    kbuf[me] = k_ref[:, wide_at(row_of, wide)]
    vbuf[me] = v_ref[:, wide_at(row_of, value_size)]
    for ds in range(1, n_part):
        for copy in kv_own(ds):
            copy.start()
    for d in range(1, n_head):
        for copy in kv_first(d):
            copy.start()
    for d in range(n_head):
        if d > 0:
            q_copy(d).start()
        else:

            @pl.when(my_group != part)
            def _():
                q_copy(0).start()

            @pl.when(my_group == part)
            def _():
                qbuf[row_of] = q_ref[:, wide_at(row_of, wide)]

    def block_of(r, group):
        return r * n_part + group + lax.rem(r, 2) * (n_part - 1 - 2 * group)

    def kv_wait(n):
        for copy in kv_copies(kbuf.at[n], vbuf.at[n], n, n, 0):
            copy.wait_recv()

    def kv_forward():
        for d in range(1, n_head):
            r = lax.rem(row_of + d, n_head)
            kv_wait(r * n_part + part)
            for ds in range(1, n_part):
                for copy in kv_second(r, ds):
                    copy.start()

    def kv_finish():
        for d in range(n_head):
            r = lax.rem(row_of + d, n_head)
            for ds in range(1, n_part):
                kv_wait(r * n_part + lax.rem(part + ds, n_part))

            @pl.when(block_of(r, part) != me)
            def _():
                remote(qbuf.at[r], qbuf.at[r], q_send.at[0], q_recv.at[r], me, sib).wait_recv()

    def o_copy(r):
        return remote(
            hsend.at[r],
            heads.at[:, wide_at(tp * n_head + row_of, value_size)],
            o_send.at[r],
            o_recv.at[row_of],
            block_of(r, part),
            tp,
        )

    score_scale = (wide // 2) ** (-0.5)

    def attend(r, carry):
        block = block_of(r, part)
        q = qbuf[r].astype(jnp.float32) * score_scale
        lane = lax.broadcasted_iota(jnp.int32, q.shape, 1)
        qtwo[0:row_count] = jnp.where(lane < wide // 2, q, 0.0).astype(jnp.bfloat16)
        qtwo[row_count:] = jnp.where(lane >= wide // 2, q, 0.0).astype(jnp.bfloat16)

        def scores_of(n):
            return lax.dot_general(
                qtwo[...], kbuf[n], (((1,), (1,)), ((), ())), preferred_element_type=jnp.float32
            )

        scores = scores_of(block)
        query = lax.broadcasted_iota(jnp.int32, scores.shape, 0)
        query = jnp.where(query >= row_count, query - row_count, query)
        key = lax.broadcasted_iota(jnp.int32, scores.shape, 1)
        scores = jnp.where(query >= key, scores, LOWEST)
        top = jnp.max(scores, axis=-1, keepdims=True)
        terms = jnp.exp(scores - top)
        total = jnp.sum(terms, axis=-1, keepdims=True)
        weighted = jnp.dot(
            terms.astype(jnp.bfloat16), vbuf[block], preferred_element_type=jnp.float32
        )

        def update(n, state):
            top, total, weighted = state
            scores = scores_of(n)
            new_top = jnp.maximum(top, jnp.max(scores, axis=-1, keepdims=True))
            terms = jnp.exp(scores - new_top)
            factor = jnp.exp(top - new_top)
            total = total * factor + jnp.sum(terms, axis=-1, keepdims=True)
            weighted = weighted * factor + jnp.dot(
                terms.astype(jnp.bfloat16), vbuf[n], preferred_element_type=jnp.float32
            )
            return (new_top, total, weighted)

        top, total, weighted = lax.fori_loop(0, block, update, (top, total, weighted))
        mapped = weighted / total
        difference = mapped[0:row_count] - scale_ref[row_of] * mapped[row_count:]
        inv_norm = lax.rsqrt(jnp.mean(difference * difference, axis=-1, keepdims=True) + EPSILON)
        result = (difference * inv_norm * gain_ref[...]).astype(jnp.bfloat16)

        @pl.when(block != me)
        def _():
            hsend[r] = result
            o_copy(r).start()

        @pl.when(block == me)
        def _():
            heads[:, wide_at(tp * n_head + row_of, value_size)] = result

        return carry

    def g_copy(t, to, k):
        return remote(heads.at[:, lanes(t)], heads.at[:, lanes(t)], g_send.at[k], g_recv.at[t], me, to)

    def heads_out():
        for d in range(n_head):
            r = lax.rem(row_of + d, n_head)

            @pl.when(r * n_part + my_group != me)
            def _():
                at = wide_at(tp * n_head + r, value_size)
                remote(heads.at[:, at], heads.at[:, at], o_send.at[0], o_recv.at[r], me, sib).wait_recv()

        for dy in range(1, n_y):
            g_copy(tp, lax.rem(my_y + dy, n_y) * 2 + core, dy - 1).start()
        g_copy(tp, sib, n_y - 1).start()

    def heads_in():
        for dy in range(1, n_y):
            t = lax.rem(my_y + n_y - dy, n_y) * 2 + core
            g_copy(t, t, 0).wait_recv()
            g_copy(t, sib, n_y - 1 + dy).start()
        g_copy(sib, sib, 0).wait_recv()
        for dy in range(1, n_y):
            g_copy(lax.rem(my_y + n_y - dy, n_y) * 2 + 1 - core, sib, 0).wait_recv()
        mixed_ref[...] = jnp.dot(
            heads[...], mix_ref[...], preferred_element_type=jnp.float32
        ).astype(jnp.bfloat16)

    def b_copy(p, t, to, k):
        return remote(
            arr.at[p, :, lanes(t)], arr.at[p, :, lanes(t)], b_send.at[p, k], b_recv.at[p, t], me, to
        )

    def gather_pair(p):
        for h in range(2):
            n = p * 2 + h

            @pl.when(n != me)
            def _():
                a_copy(n, n).wait_recv()

        for dy in range(1, n_y):
            to = lax.rem(my_y + dy, n_y) * 2 + core
            b_copy(p, tp, to, dy - 1).start()
        b_copy(p, tp, sib, n_y - 1).start()

    def forward_pair(p):
        for dy in range(1, n_y):
            t = lax.rem(my_y + n_y - dy, n_y) * 2 + core
            b_copy(p, t, t, 0).wait_recv()
            b_copy(p, t, sib, n_y - 1 + dy).start()
        b_copy(p, sib, sib, 0).wait_recv()
        for dy in range(1, n_y):
            t = lax.rem(my_y + n_y - dy, n_y) * 2 + 1 - core
            b_copy(p, t, sib, 0).wait_recv()

    ff = gate_ref.shape[1]
    tile = min(256, ff)

    def s_copy(p):
        return remote(sib_send.at[p], sib_recv.at[p], s_send.at[p], s_recv.at[p], me, sib)

    def y_copy(p, dy):
        to = lax.rem(my_y + dy, n_y) * 2 + core
        return remote(
            y_send.at[p, dy - 1], y_recv.at[p, dy - 1], y_ssem.at[p, dy - 1], y_rsem.at[p, dy - 1], me, to
        )

    def compute(p):
        def up_tile(f, carry):
            at = pl.ds(pl.multiple_of(f * tile, tile), tile)
            x = arr[p]
            gate = jnp.dot(x, gate_ref[:, at], preferred_element_type=jnp.float32)
            up = jnp.dot(x, up_ref[:, at], preferred_element_type=jnp.float32)
            hidden[:, at] = (gate / (1.0 + jnp.exp(-gate)) * up).astype(jnp.bfloat16)
            return carry

        lax.fori_loop(0, ff // tile, up_tile, 0)

        def sib_tile(y, carry):
            part = jnp.dot(
                hidden[...], down_ref[:, lanes(y * 2 + 1 - core)], preferred_element_type=jnp.float32
            )
            sib_send[p, y] = part.astype(jnp.bfloat16)
            return carry

        lax.fori_loop(0, n_y, sib_tile, 0)
        s_copy(p).start()

        def own_tile(y, carry):
            own_sum[p, y] = jnp.dot(
                hidden[...], down_ref[:, lanes(y * 2 + core)], preferred_element_type=jnp.float32
            )
            return carry

        lax.fori_loop(0, n_y, own_tile, 0)

    def chip_sum(p):
        s_copy(p).wait_recv()
        for dy in range(1, n_y):
            y = lax.rem(my_y + dy, n_y)
            y_send[p, dy - 1] = (own_sum[p, y] + sib_recv[p, y].astype(jnp.float32)).astype(jnp.bfloat16)
            y_copy(p, dy).start()

    def r_copy(dest, src_n):
        return remote(
            answer.at[dest // 2, rows(lax.rem(dest, 2))], ret_ref.at[src_n], r_send.at[dest], r_recv.at[src_n], dest, tp
        )

    def give_back(p):
        total = own_sum[p, my_y] + sib_recv[p, my_y].astype(jnp.float32)
        for dy in range(1, n_y):
            y_copy(p, dy).wait_recv()
            total = total + y_recv[p, dy - 1].astype(jnp.float32)
        answer[p] = total.astype(jnp.bfloat16)
        for h in range(2):
            dest = p * 2 + h

            @pl.when(dest != me)
            def _():
                r_copy(dest, me).start()

            @pl.when(dest == me)
            def _():
                ret_ref[me] = answer[my_pair, rows(half)]

    def pair_of(d):
        return lax.rem(my_pair + d + pairs, pairs)

    def step(i, carry):
        @pl.when(i < pairs)
        def _():
            gather_pair(pair_of(i))

        @pl.when(jnp.logical_and(i >= LAG, i < pairs + LAG))
        def _():
            p = pair_of(i - LAG)
            forward_pair(p)

            @pl.when(i == LAG)
            def _():
                for copy in weights:
                    copy.wait()

            compute(p)

        @pl.when(i >= LAG + 1)
        def _():
            chip_sum(pair_of(i - LAG - 1))

        @pl.when(i >= LAG + 2)
        def _():
            give_back(pair_of(i - LAG - 2))

        return carry

    lax.fori_loop(0, pairs + LAG, step, 0)
    chip_sum(pair_of(pairs - 1))
    kv_forward()
    give_back(pair_of(pairs - 2))
    kv_finish()
    lax.fori_loop(0, n_head, attend, 0)
    give_back(pair_of(pairs - 1))
    heads_out()
    heads_in()

    for d in range(n_head):
        if d > 0:
            for copy in kv_first(d):
                copy.wait_send()
            q_copy(d).wait_send()
        for ds in range(1, n_part):
            for copy in kv_second(lax.rem(row_of + d, n_head), ds):
                copy.wait_send()

        @pl.when(block_of(d, part) != me)
        def _():
            o_copy(d).wait_send()

    @pl.when(my_group != part)
    def _():
        q_copy(0).wait_send()

    for k in range(n_tp - 1):
        g_copy(tp, sib, k).wait_send()

    def drain(d, carry):
        p = pair_of(d)
        for k in range(n_tp - 1):
            b_copy(p, tp, sib, k).wait_send()
        s_copy(p).wait_send()
        for dy in range(1, n_y):
            y_copy(p, dy).wait_send()
        for h in range(2):
            n = p * 2 + h

            @pl.when(n != me)
            def _():
                a_copy(n, n).wait_send()
                r_copy(n, n).wait()

        return carry

    lax.fori_loop(0, pairs, drain, 0)


LAG = 1


def fused(outgoing, queries, key_rows, values, second_scale, head_gain, out_weight, gate_weight, up_weight, down_weight):
    n_ep, cap, cols = outgoing.shape
    n_tp = lax.axis_size("tp")
    width, ff = gate_weight.shape[1:]
    pairs, n_y = n_ep // 2, n_tp // 2
    n_head, rows = second_scale.shape[0], queries.shape[0]
    n_part = n_ep // n_head
    wide, value_size = queries.shape[1] // n_head, values.shape[1] // n_head
    bf, dma = jnp.bfloat16, pltpu.SemaphoreType.DMA
    return pl.pallas_call(
        functools.partial(fused_kernel, (n_ep, n_tp, cap, cols, n_head)),
        out_shape=(
            jax.ShapeDtypeStruct((n_ep, cap, cols), bf),
            jax.ShapeDtypeStruct((rows, out_weight.shape[1]), bf),
        ),
        in_specs=[pl.BlockSpec(memory_space=pltpu.VMEM)] * 4
        + [pl.BlockSpec(memory_space=pltpu.SMEM), pl.BlockSpec(memory_space=pltpu.VMEM)]
        + [pl.BlockSpec(memory_space=pl.ANY)] * 4,
        out_specs=(pl.BlockSpec(memory_space=pltpu.VMEM),) * 2,
        scratch_shapes=[
            pltpu.VMEM((width, ff), bf),
            pltpu.VMEM((width, ff), bf),
            pltpu.VMEM((ff, width), bf),
            pltpu.VMEM((pairs, 2 * cap, width), bf),
            pltpu.VMEM((2 * cap, ff), bf),
            pltpu.VMEM((pairs, n_y, 2 * cap, cols), jnp.float32),
            pltpu.VMEM((pairs, n_y, 2 * cap, cols), bf),
            pltpu.VMEM((pairs, n_y, 2 * cap, cols), bf),
            pltpu.VMEM((pairs, n_y - 1, 2 * cap, cols), bf),
            pltpu.VMEM((pairs, n_y - 1, 2 * cap, cols), bf),
            pltpu.VMEM((pairs, 2 * cap, cols), bf),
            dma((4,)),
            dma((n_ep,)),
            dma((n_ep,)),
            dma((pairs, n_tp - 1)),
            dma((pairs, n_tp)),
            dma((pairs,)),
            dma((pairs,)),
            dma((pairs, n_y - 1)),
            dma((pairs, n_y - 1)),
            dma((n_ep,)),
            dma((n_ep,)),
            pltpu.VMEM(out_weight.shape, bf),
            pltpu.VMEM((n_ep, rows, wide), bf),
            pltpu.VMEM((n_ep, rows, value_size), bf),
            pltpu.VMEM((n_head, rows, wide), bf),
            pltpu.VMEM((2 * rows, wide), bf),
            pltpu.VMEM((n_head, rows, value_size), bf),
            pltpu.VMEM((rows, n_tp * n_head * value_size), bf),
            dma((2, n_head + n_head * (n_part - 1))),
            dma((2, n_ep)),
            dma((n_head,)),
            dma((n_head,)),
            dma((n_head,)),
            dma((n_head,)),
            dma((n_tp - 1,)),
            dma((n_tp,)),
        ],
        compiler_params=pltpu.CompilerParams(
            collective_id=0, has_side_effects=True, vmem_limit_bytes=56 * 1024 * 1024
        ),
    )(
        outgoing,
        queries,
        key_rows,
        values,
        second_scale,
        head_gain.reshape(1, -1),
        out_weight,
        gate_weight,
        up_weight,
        down_weight,
    )


def local(
    queries,
    key_rows,
    values,
    second_scale,
    head_gain,
    out_weight,
    routed_in,
    routed_gain,
    expert_ids,
    group_logits,
    inner_logits,
    gate_weight,
    up_weight,
    down_weight,
):
    token_count, width = routed_in.shape
    chosen = expert_ids.shape[1]
    ep_size = lax.axis_size("ep")
    capacity = 2 * chosen * token_count // ep_size
    source = routed_in.astype(jnp.float32)
    inv_norm = lax.rsqrt(jnp.mean(source * source, axis=-1, keepdims=True) + EPSILON)
    columns = width // lax.axis_size("tp")
    first = lax.axis_index("tp") * columns
    own_source = lax.dynamic_slice_in_dim(routed_in, first, columns, 1).astype(jnp.float32)
    own_gain = lax.dynamic_slice_in_dim(routed_gain, first, columns, 0)
    normed = (own_source * inv_norm * own_gain).astype(jnp.bfloat16)
    experts = jnp.arange(ep_size, dtype=jnp.int32)
    picks = expert_ids[..., None] == experts
    picked = jnp.any(picks, axis=1)
    positions = jnp.arange(token_count, dtype=jnp.int32)
    before = (positions[:, None] > positions[None, :]).astype(jnp.bfloat16)
    slot = jnp.dot(before, picked.astype(jnp.bfloat16), preferred_element_type=jnp.float32)
    slot = jnp.where(picked, slot.astype(jnp.int32), -1)
    slots = jnp.arange(capacity, dtype=jnp.int32)
    place = slot.T[:, None, :] == slots[None, :, None]
    spread = place.reshape(ep_size * capacity, token_count).astype(jnp.bfloat16)
    outgoing = jnp.dot(spread, normed, preferred_element_type=jnp.float32).astype(jnp.bfloat16)
    returned, mixer_out = fused(
        outgoing.reshape(ep_size, capacity, columns),
        queries,
        key_rows,
        values,
        second_scale,
        head_gain,
        out_weight,
        gate_weight,
        up_weight,
        down_weight,
    )
    group_prob = jax.nn.softmax(group_logits, axis=-1)
    member = (
        expert_ids[..., None] // GROUP_SIZE == jnp.arange(group_logits.shape[1], dtype=jnp.int32)
    ).astype(jnp.float32)
    group_pick = jnp.sum(group_prob[:, None, :] * member, axis=-1)
    route_weight = group_pick * jax.nn.softmax(inner_logits, axis=-1)
    expert_weight = jnp.sum(route_weight[..., None] * picks.astype(jnp.float32), axis=1)
    high = expert_weight.astype(jnp.bfloat16)
    low = (expert_weight - high.astype(jnp.float32)).astype(jnp.bfloat16)
    back = slot[:, :, None] == slots[None, None, :]

    def combine(weight):
        mix = jnp.where(back, weight[:, :, None], jnp.bfloat16(0)).reshape(token_count, -1)
        return jnp.dot(mix, returned.reshape(-1, columns), preferred_element_type=jnp.float32)

    return (mixer_out, (combine(high) + combine(low)).astype(jnp.bfloat16))


def solution(mesh):
    return jax.shard_map(
        local,
        mesh=mesh,
        in_specs=(
            P("ep", "tp"),
            P("ep", "tp"),
            P("ep", "tp"),
            P("tp"),
            P(),
            P(None, "tp"),
            P("ep", None),
            P(),
            P("ep", None),
            P("ep", None),
            P("ep", None),
            P("ep", None, "tp"),
            P("ep", None, "tp"),
            P("ep", "tp", None),
        ),
        out_specs=(P("ep", "tp"), P("ep", "tp")),
        check_vma=False,
    )
```
